32 devices in a mesh: sp: 8 (over z, x), tp: 4 (over y, core).
Axes of the slice: x: 2, y: 2, z: 4, core: 2. Of those that a mesh axis runs over, the one named last changes fastest.
Arguments:
- query_small: bfloat16 [6144, 1024], P('sp', 'tp'), may hold values from -18 to 18
- key_small: bfloat16 [6144, 1024], P('sp', 'tp'), may hold values from -6 to 6
- value_small: bfloat16 [6144, 1024], P('sp', 'tp'), may hold values from -6 to 6
- offset_small: bfloat16 [16, 6144], P('tp', 'sp'), may hold values from -25 to 0
- query_large: bfloat16 [6144, 1024], P('sp', 'tp'), may hold values from -18 to 18
- key_large: bfloat16 [6144, 1024], P('sp', 'tp'), may hold values from -6 to 6
- value_large: bfloat16 [6144, 1024], P('sp', 'tp'), may hold values from -6 to 6
- offset_large: bfloat16 [8, 6144], P('tp', 'sp'), may hold values from -25 to 0
- out_small: bfloat16 [1024, 2048], P('tp'), may hold values from -0.125 to 0.125
- out_large: bfloat16 [1024, 2048], P('tp'), may hold values from -0.125 to 0.125
- residual: bfloat16 [6144, 2048], P(('sp', 'tp')), may hold values from -1.1953125 to 1.1953125
- norm_gain: bfloat16 [2048], replicated, may hold values from 0.099609375 to 1.8984375
- gate_weight: bfloat16 [2048, 5632], P('sp', 'tp'), may hold values from -0.125 to 0.125
- up_weight: bfloat16 [2048, 5632], P('sp', 'tp'), may hold values from -0.125 to 0.125
- down_weight: bfloat16 [5632, 2048], P('tp', 'sp'), may hold values from -0.078125 to 0.078125
Outputs:
- layer_out: bfloat16 [6144, 2048], P(('sp', 'tp'))
The draws below stay inside these ranges and needn't reach their ends.
All inputs are finite; a program needn't handle non-finite values.
Results may differ from the reference program's by a relative error of at most 0.023.
Values may be sent and summed in bfloat16 or wider, within the bound.
A program may use at most 128 MiB of HBM per device.

```python
import math
import jax
import jax.numpy as jnp
from jax import lax

D = 2048
HEADS_SMALL = 16
SMALL_DIM = 64
HEADS_LARGE = 8
LARGE_DIM = 128
FF = 5632
TOK_DEV = 768
SEQUENCE_LENGTH = 6144
N_TP = 4


def draw_offsets(key, head_count_list):
    random_keys = jax.random.split(key, 7)
    share = 0.5
    quick = jax.random.uniform(random_keys[0], (head_count_list,)) < share
    slow_base = math.log(0.35 / SEQUENCE_LENGTH) - 4.5 + jax.random.uniform(random_keys[1], (head_count_list,), minval=-0.5, maxval=0.5)
    quick_base = -8.4 + jax.random.uniform(random_keys[2], (head_count_list,), minval=-0.5, maxval=0.5)
    baseline_output = jnp.where(quick, quick_base, slow_base)
    position_shifts = jax.random.uniform(random_keys[3], (head_count_list, SEQUENCE_LENGTH // TOK_DEV), minval=-0.7, maxval=0.7)
    position_shifts = jnp.repeat(position_shifts, TOK_DEV, axis=1)
    approximate_output = jax.random.uniform(random_keys[4], (head_count_list, SEQUENCE_LENGTH), minval=-0.5, maxval=0.5)
    sample_spots = jax.random.randint(random_keys[5], (head_count_list, 3), 0, SEQUENCE_LENGTH)
    token_places = jnp.arange(SEQUENCE_LENGTH, dtype=jnp.int32)
    sample_draw = jnp.any(token_places[None, :, None] == sample_spots[:, None, :], axis=2)
    sample_draw_value = jax.random.uniform(random_keys[6], (head_count_list, SEQUENCE_LENGTH), minval=-1.5, maxval=-0.5)
    return jnp.where(sample_draw, sample_draw_value, baseline_output[:, None] + position_shifts + approximate_output).astype(jnp.float32)


def draw_offset_small(key, part):
    return draw_offsets(jax.random.fold_in(key, 11), HEADS_SMALL).astype(jnp.bfloat16)


def draw_offset_large(key, part):
    return draw_offsets(jax.random.fold_in(key, 23), HEADS_LARGE).astype(jnp.bfloat16)


def level_of(rng, extent, shards, least, largest):
    def one(dim, parts):
        steps = jax.random.uniform(jax.random.fold_in(jax.random.fold_in(rng, 6), dim), (parts,), jnp.float32, least / len(shards), largest / len(shards))
        return jnp.repeat(jnp.exp(steps), extent[dim] // parts).reshape((-1,) + (1,) * (len(extent) - dim - 1))

    factor_of = one(*shards[0])
    for cut in shards[1:]:
        factor_of = factor_of * one(*cut)
    return factor_of


def normal_values(rng, extent, width, limit, pieces=(), kind=jnp.bfloat16):
    result = width * jax.random.normal(rng, extent, jnp.float32)
    if pieces:
        result = result * level_of(rng, extent, pieces, -0.22, 0.18)
    return jnp.clip(result, -limit, limit).astype(kind)


def setup_inputs(seed: int = 0) -> dict:
    seeds = jax.random.split(jax.random.key(seed), 16)
    query_small = normal_values(seeds[0], (SEQUENCE_LENGTH, HEADS_SMALL * SMALL_DIM), 3.0, 18.0, ((0, 8), (1, 4)))
    key_small = normal_values(seeds[1], (SEQUENCE_LENGTH, HEADS_SMALL * SMALL_DIM), 1.0, 6.0, ((0, 8), (1, 4)))
    value_small = normal_values(seeds[2], (SEQUENCE_LENGTH, HEADS_SMALL * SMALL_DIM), 1.0, 6.0, ((0, 8), (1, 4)))
    offset_small = draw_offset_small(jax.random.fold_in(seeds[15], 71), 0)
    query_large = normal_values(seeds[4], (SEQUENCE_LENGTH, HEADS_LARGE * LARGE_DIM), 3.0, 18.0, ((0, 8), (1, 4)))
    key_large = normal_values(seeds[5], (SEQUENCE_LENGTH, HEADS_LARGE * LARGE_DIM), 1.0, 6.0, ((0, 8), (1, 4)))
    value_large = normal_values(seeds[6], (SEQUENCE_LENGTH, HEADS_LARGE * LARGE_DIM), 1.0, 6.0, ((0, 8), (1, 4)))
    offset_large = draw_offset_large(jax.random.fold_in(seeds[15], 71), 0)
    out_small = normal_values(seeds[8], (HEADS_SMALL * SMALL_DIM, D), (HEADS_SMALL * SMALL_DIM + HEADS_LARGE * LARGE_DIM) ** -0.5, 0.125, ((0, 4),))
    out_large = normal_values(seeds[9], (HEADS_LARGE * LARGE_DIM, D), (HEADS_SMALL * SMALL_DIM + HEADS_LARGE * LARGE_DIM) ** -0.5, 0.125, ((0, 4),))
    residual = normal_values(seeds[10], (SEQUENCE_LENGTH, D), 0.2, 1.1953125, ((0, 32),))
    norm_gain = jnp.clip(1.0 + 0.18 * jax.random.normal(seeds[11], (D,), jnp.float32), 0.099609375, 1.8984375).astype(jnp.bfloat16)
    gate_weight = normal_values(seeds[12], (D, FF), D ** -0.5, 0.125, ((0, 8), (1, 4)))
    up_weight = normal_values(seeds[13], (D, FF), D ** -0.5, 0.125, ((0, 8), (1, 4)))
    down_weight = normal_values(seeds[14], (FF, D), FF ** -0.5, 0.078125, ((0, 4), (1, 8)))
    return {"query_small": query_small, "key_small": key_small, "value_small": value_small, "offset_small": offset_small, "query_large": query_large, "key_large": key_large, "value_large": value_large, "offset_large": offset_large, "out_small": out_small, "out_large": out_large, "residual": residual, "norm_gain": norm_gain, "gate_weight": gate_weight, "up_weight": up_weight, "down_weight": down_weight}


def stick_group(query, random_keys, values, offset, head_depth):
    head_count_list = offset.shape[0]

    def per_head(args):
        head_query, head_keys, head_values, head_offset = args
        key_pos = jnp.arange(SEQUENCE_LENGTH, dtype=jnp.int32)

        def per_block(first_row):
            block_query = lax.dynamic_slice_in_dim(head_query, first_row, TOK_DEV, 0)
            logits = jnp.dot(block_query, head_keys.T, preferred_element_type=jnp.float32) * head_depth ** (-0.5)
            logits = logits + head_offset.astype(jnp.float32)[None, :]
            query_pos = first_row + jnp.arange(TOK_DEV, dtype=jnp.int32)
            before = key_pos[None, :] < query_pos[:, None]
            fail_all = jax.nn.log_sigmoid(-logits)
            log_pass = logits + fail_all
            log_fail = jnp.where(before, fail_all, 0.0)
            suffix = lax.cumsum(log_fail, axis=1, reverse=True) - log_fail
            weights = jnp.where(before, jnp.exp(log_pass + suffix), 0.0).astype(jnp.bfloat16)
            return jnp.dot(weights, head_values, preferred_element_type=jnp.float32).astype(jnp.bfloat16)
        starts = jnp.arange(SEQUENCE_LENGTH // TOK_DEV, dtype=jnp.int32) * TOK_DEV
        return lax.map(per_block, starts).reshape(SEQUENCE_LENGTH, head_depth)

    def split_heads(flat):
        return flat.reshape(SEQUENCE_LENGTH, head_count_list, head_depth).transpose(1, 0, 2)
    mixed = lax.map(per_head, (split_heads(query), split_heads(random_keys), split_heads(values), offset))
    return mixed.transpose(1, 0, 2).reshape(SEQUENCE_LENGTH, head_count_list * head_depth)

def rounded(value):
    return lax.optimization_barrier(value.astype(jnp.bfloat16)).astype(jnp.float32)

def reference(query_small, key_small, value_small, offset_small, query_large, key_large, value_large, offset_large, out_small, out_large, residual, norm_gain, gate_weight, up_weight, down_weight):
    mixed_small = stick_group(query_small, key_small, value_small, offset_small, SMALL_DIM)
    mixed_large = stick_group(query_large, key_large, value_large, offset_large, LARGE_DIM)
    small_run = HEADS_SMALL * SMALL_DIM // N_TP
    large_run = HEADS_LARGE * LARGE_DIM // N_TP
    total = jnp.zeros((SEQUENCE_LENGTH, D), jnp.float32)
    for group in range(N_TP):
        part = jnp.dot(mixed_small[:, group * small_run:(group + 1) * small_run], out_small[group * small_run:(group + 1) * small_run], preferred_element_type=jnp.float32)
        part = part + jnp.dot(mixed_large[:, group * large_run:(group + 1) * large_run], out_large[group * large_run:(group + 1) * large_run], preferred_element_type=jnp.float32)
        total = total + rounded(part)
    stream = residual.astype(jnp.float32) + rounded(total)
    scale = lax.rsqrt(lax.optimization_barrier(jnp.mean(stream * stream, axis=-1, keepdims=True)) + 1e-06)
    normed = (stream * scale * norm_gain.astype(jnp.float32)).astype(jnp.bfloat16)
    gate = jnp.dot(normed, gate_weight, preferred_element_type=jnp.float32)
    upper = jnp.dot(normed, up_weight, preferred_element_type=jnp.float32)
    hidden = (jax.nn.silu(gate) * upper).astype(jnp.bfloat16)
    hidden_run = FF // N_TP
    summed = jnp.zeros((SEQUENCE_LENGTH, D), jnp.float32)
    for group in range(N_TP):
        part = jnp.dot(hidden[:, group * hidden_run:(group + 1) * hidden_run], down_weight[group * hidden_run:(group + 1) * hidden_run], preferred_element_type=jnp.float32)
        summed = summed + rounded(part)
    return (stream + rounded(summed)).astype(jnp.bfloat16)
```

```python
import math

import jax
import jax.numpy as jnp
from jax import lax
from jax.experimental import pallas as pl
from jax.experimental.pallas import tpu as pltpu
from jax.sharding import PartitionSpec as P


SMALL_DIM = 64
LARGE_DIM = 128
TILE = 256
LANES = 128
LOG2E = math.log2(math.e)


def dot_t(a, b):
    return lax.dot_general(a, b, (((1,), (1,)), ((), ())), preferred_element_type=jnp.float32)


def attend_kernel(
    sp_ref, q_ref, k_small, v_small, k_large, v_large, off_ref, tri_ref, out_ref, qs_ref, acc_ref, carry_ref
):
    tokens = q_ref.shape[0] * pl.num_programs(0)
    small_cols = k_small.shape[1]
    n_small = small_cols // SMALL_DIM
    n_large = k_large.shape[1] // LARGE_DIM
    n_pairs = small_cols // LANES
    lane = lax.broadcasted_iota(jnp.int32, (TILE, LANES), 1)
    low = lane < SMALL_DIM
    zero = jnp.zeros((TILE, LANES), jnp.bfloat16)
    for pair in range(n_pairs):
        q = q_ref[:, pair * LANES : (pair + 1) * LANES]
        qs_ref[2 * pair] = jnp.where(low, q, zero)
        qs_ref[2 * pair + 1] = jnp.where(low, zero, q)
    for head in range(n_large):
        first = small_cols + head * LANES
        qs_ref[n_small + head] = q_ref[:, first : first + LANES]
    acc_ref[...] = jnp.zeros_like(acc_ref)
    carry_ref[...] = jnp.zeros_like(carry_ref)
    tri = tri_ref[...]
    diagonal = sp_ref[0] * (tokens // TILE) + pl.program_id(0)

    def weights_of(head, key, tile, scale, before):
        z = dot_t(qs_ref[head], key) * scale + off_ref[head, tile]
        t = jnp.log(1.0 + jnp.exp2(-jnp.abs(z))) * LOG2E
        log_pass = jnp.minimum(z, 0.0) - t
        log_fail = log_pass - z
        if before is not None:
            log_fail = jnp.where(before, log_fail, 0.0)
        after = jnp.dot(log_fail.astype(jnp.bfloat16), tri, preferred_element_type=jnp.float32)
        carried = carry_ref[head]
        weights = jnp.exp2(log_pass + after + carried)
        if before is not None:
            weights = jnp.where(before, weights, 0.0)
        carry_ref[head] = carried + after[:, :1] + log_fail[:, :1]
        return weights.astype(jnp.bfloat16)

    def one_tile(tile, before):
        rows = pl.ds(pl.multiple_of(tile * TILE, TILE), TILE)
        for pair in range(n_pairs):
            cols = slice(pair * LANES, (pair + 1) * LANES)
            key = k_small[rows, cols]
            value = v_small[rows, cols]
            scale = LOG2E * SMALL_DIM**-0.5
            w0 = weights_of(2 * pair, key, tile, scale, before)
            w1 = weights_of(2 * pair + 1, key, tile, scale, before)
            acc_ref[:, cols] += jnp.dot(
                w0, jnp.where(low, value, zero), preferred_element_type=jnp.float32
            ) + jnp.dot(w1, jnp.where(low, zero, value), preferred_element_type=jnp.float32)
        for head in range(n_large):
            cols = slice(head * LANES, (head + 1) * LANES)
            out_cols = slice(small_cols + head * LANES, small_cols + (head + 1) * LANES)
            w = weights_of(
                n_small + head, k_large[rows, cols], tile, LOG2E * LARGE_DIM**-0.5, before
            )
            acc_ref[:, out_cols] += jnp.dot(
                w, v_large[rows, cols], preferred_element_type=jnp.float32
            )

    row_pos = lax.broadcasted_iota(jnp.int32, (TILE, TILE), 0)
    key_pos = lax.broadcasted_iota(jnp.int32, (TILE, TILE), 1)
    one_tile(diagonal, key_pos < row_pos)

    def step(index, nothing):
        one_tile(diagonal - 1 - index, None)
        return nothing

    lax.fori_loop(0, diagonal, step, 0)
    out_ref[...] = acc_ref[...].astype(jnp.bfloat16)


def attend(sp_index, query, k_small, v_small, k_large, v_large, offsets):
    tokens, cols = query.shape
    heads, length = offsets.shape
    off = (offsets.astype(jnp.float32) * LOG2E).reshape(heads, length // TILE, 1, TILE)
    places = jnp.arange(TILE, dtype=jnp.int32)
    tri = (places[:, None] > places[None, :]).astype(jnp.bfloat16)
    whole = pl.BlockSpec(memory_space=pltpu.VMEM)
    return pl.pallas_call(
        attend_kernel,
        out_shape=jax.ShapeDtypeStruct((tokens, cols), jnp.bfloat16),
        grid=(tokens // TILE,),
        in_specs=[
            pl.BlockSpec(memory_space=pltpu.SMEM),
            pl.BlockSpec((TILE, cols), lambda i: (i, 0)),
            whole,
            whole,
            whole,
            whole,
            whole,
            whole,
        ],
        out_specs=pl.BlockSpec((TILE, cols), lambda i: (i, 0)),
        scratch_shapes=[
            pltpu.VMEM((heads, TILE, LANES), jnp.bfloat16),
            pltpu.VMEM((TILE, cols), jnp.float32),
            pltpu.VMEM((heads, TILE, 1), jnp.float32),
        ],
        compiler_params=pltpu.CompilerParams(vmem_limit_bytes=60 * 1024 * 1024),
        cost_estimate=pl.CostEstimate(
            flops=2 * 3 * heads * tokens * length * TILE,
            bytes_accessed=8 * length * cols,
            transcendentals=3 * heads * tokens * length,
        ),
        name="stick_attend",
    )(sp_index.reshape(1).astype(jnp.int32), query, k_small, v_small, k_large, v_large, off, tri)


def rounded(value):
    return lax.optimization_barrier(value.astype(jnp.bfloat16)).astype(jnp.float32)


def rms_norm(stream, gain):
    scale = lax.rsqrt(jnp.mean(stream * stream, axis=-1, keepdims=True) + 1e-06)
    return (stream * scale * gain.astype(jnp.float32)).astype(jnp.bfloat16)


def layer(
    query_small,
    key_small,
    value_small,
    offset_small,
    query_large,
    key_large,
    value_large,
    offset_large,
    out_small,
    out_large,
    residual,
    norm_gain,
    gate_weight,
    up_weight,
    down_weight,
):
    sp_index = lax.axis_index("sp")
    members = tuple(
        lax.all_gather(member, "sp", axis=0, tiled=True)
        for member in (key_small, value_small, key_large, value_large)
    )
    offsets = lax.all_gather(
        jnp.concatenate([offset_small, offset_large], axis=0), "sp", axis=1, tiled=True
    )
    members, offsets, gate_weight, up_weight, down_weight = lax.optimization_barrier(
        (members, offsets, gate_weight, up_weight, down_weight)
    )
    gate_full = lax.all_gather(gate_weight, "sp", axis=0, tiled=True)
    up_full = lax.all_gather(up_weight, "sp", axis=0, tiled=True)
    down_full = lax.all_gather(down_weight, "sp", axis=1, tiled=True)
    query = jnp.concatenate([query_small, query_large], axis=1)
    out_rows = jnp.concatenate([out_small, out_large], axis=0)
    mixed = attend(sp_index, query, *members, offsets)
    attended = lax.psum_scatter(
        jnp.dot(mixed, out_rows, preferred_element_type=jnp.float32).astype(jnp.bfloat16),
        "tp",
        scatter_dimension=0,
        tiled=True,
    ).astype(jnp.float32)
    stream = residual.astype(jnp.float32) + rounded(attended)
    normed = rms_norm(stream, norm_gain)
    normed_rows = lax.all_gather(normed, "tp", axis=0, tiled=True)
    gate = jnp.dot(normed_rows, gate_full, preferred_element_type=jnp.float32)
    upper = jnp.dot(normed_rows, up_full, preferred_element_type=jnp.float32)
    hidden = (jax.nn.silu(gate) * upper).astype(jnp.bfloat16)
    summed = lax.psum_scatter(
        jnp.dot(hidden, down_full, preferred_element_type=jnp.float32).astype(jnp.bfloat16),
        "tp",
        scatter_dimension=0,
        tiled=True,
    ).astype(jnp.float32)
    return (stream + rounded(summed)).astype(jnp.bfloat16)


def solution(mesh):
    return jax.shard_map(
        layer,
        mesh=mesh,
        in_specs=(
            P("sp", "tp"),
            P("sp", "tp"),
            P("sp", "tp"),
            P("tp", "sp"),
            P("sp", "tp"),
            P("sp", "tp"),
            P("sp", "tp"),
            P("tp", "sp"),
            P("tp", None),
            P("tp", None),
            P(("sp", "tp"), None),
            P(),
            P("sp", "tp"),
            P("sp", "tp"),
            P("tp", "sp"),
        ),
        out_specs=P(("sp", "tp"), None),
        check_vma=False,
    )
```
